128 devices in a mesh: sp: 16 (over z, x), tp: 8 (over y, core).
Axes of the slice: x: 4, y: 4, z: 4, core: 2. Of those that a mesh axis runs over, the one named last changes fastest.
Arguments:
- residual: bfloat16 [8192, 4096], P('sp'), may hold values from -6 to 6
- queries: bfloat16 [8192, 1024], P('sp', 'tp'), may hold values from -6 to 6
- projected_key_rows: bfloat16 [8192, 1024], P('sp', 'tp'), may hold values from -6 to 6
- projected_value_rows: bfloat16 [8192, 2048], P('sp', 'tp'), may hold values from -6 to 6
- output_gate_logits: bfloat16 [8192, 2048], P('sp', 'tp'), may hold values from -6 to 6
- input_gate_logits: float32 [16, 8192], P('tp', 'sp'), may hold values from -8 to 120
- forget_gate_logits: float32 [16, 8192], P('tp', 'sp'), may hold values from 0 to 16
- extra_forget_logits: float32 [16, 8192], P('tp', 'sp'), may hold values from -0.7 to 0, as said below
- head_norm_gain: bfloat16 [2048], P('tp'), may hold values from 0.099609375 to 1.8984375
- output_projection_weight: bfloat16 [2048, 4096], P('tp'), may hold values from -0.125 to 0.125
- feedforward_norm_gain: bfloat16 [4096], replicated, may hold values from 0.099609375 to 1.8984375
- feedforward_gate_weight: bfloat16 [4096, 11264], P('sp', 'tp'), may hold values from -0.09375 to 0.09375
- up_projection_weight: bfloat16 [4096, 11264], P('sp', 'tp'), may hold values from -0.09375 to 0.09375
- down_projection_weight: bfloat16 [4096, 11264], P('sp', 'tp'), may hold values from -0.0546875 to 0.0546875
Outputs:
- layer_out: bfloat16 [8192, 4096], P(('sp', 'tp'))
The draws below stay inside these ranges and needn't reach their ends.
Inputs may be any that keep to these rules, and one draw needn't show every extreme that they name: `extra_forget_logits`: each entry is 0 or the logarithm of a factor between one half and 0.8.
All inputs are finite; a program needn't handle non-finite values.
Results may differ from the reference program's by a relative error of at most 0.01.
Values may be sent and summed in bfloat16 or wider, within the bound.
A program may use at most 192 MiB of HBM per device.

```python
import math
import jax
import jax.numpy as jnp
from jax import lax

D = 4096
HEADS = 16
QK_DIM = 64
V_DIM = 128
FF = 11264
BLOCK = 64
TOK_DEV = 512
TOKENS = 8192
VW = 2048
N_TP = 8


def draw_input_gate_logits(key, part):
    values = jnp.clip(1.5 * jax.random.normal(jax.random.fold_in(key, 11), (HEADS, TOKENS), jnp.float32), -6.0, 6.0)
    return values.astype(jnp.float32)


def draw_forget_gate_logits(key, part):
    slow = jax.random.bernoulli(jax.random.fold_in(key, 21), 0.5, (HEADS, 1))
    noise = 0.7 * jax.random.normal(jax.random.fold_in(key, 22), (HEADS, TOKENS), jnp.float32)
    base = jnp.where(slow, math.log(TOKENS) + 1.5, 3.5)
    shift = jax.random.uniform(jax.random.fold_in(key, 23), (HEADS, TOKENS // TOK_DEV), jnp.float32, -0.7, 0.7)
    values = base + noise + jnp.repeat(shift, TOK_DEV, axis=1)
    return jnp.clip(values, 0.0, 16.0).astype(jnp.float32)


def draw_extra_forget_logits(key, part):
    hits = jax.random.bernoulli(jax.random.fold_in(key, 31), 4.0 / TOKENS, (HEADS, TOKENS))
    factor = jax.random.uniform(jax.random.fold_in(key, 32), (HEADS, TOKENS), jnp.float32, 0.5, 0.8)
    return jnp.where(hits, jnp.log(factor), 0.0).astype(jnp.float32)


def block_levels(rng, shape, split, least, top_value):
    def one(dim, parts):
        draws = jax.random.uniform(jax.random.fold_in(jax.random.fold_in(rng, 6), dim), (parts,), jnp.float32, least / len(split), top_value / len(split))
        return jnp.repeat(jnp.exp(draws), shape[dim] // parts).reshape((-1,) + (1,) * (len(shape) - dim - 1))

    level = one(*split[0])
    for cut in split[1:]:
        level = level * one(*cut)
    return level


def centred(key, extent, scale, bound, cuts=(), kind=jnp.bfloat16):
    drawn = scale * jax.random.normal(key, extent, jnp.float32)
    if cuts:
        drawn = drawn * block_levels(key, extent, cuts, -0.22, 0.18)
    return jnp.clip(drawn, -bound, bound).astype(kind)


def setup_inputs(seed: int = 0) -> dict:
    streams_of = jax.random.split(jax.random.key(seed), 15)
    residual = centred(streams_of[0], (TOKENS, D), 1.0, 6.0, ((0, 16),))
    queries = centred(streams_of[1], (TOKENS, HEADS * QK_DIM), 1.0, 6.0, ((0, 16), (1, 8)))
    projected_key_rows = centred(streams_of[2], (TOKENS, HEADS * QK_DIM), 1.0, 6.0, ((0, 16), (1, 8)))
    projected_value_rows = centred(streams_of[3], (TOKENS, VW), 1.0, 6.0, ((0, 16), (1, 8)))
    output_gate_logits = centred(streams_of[4], (TOKENS, VW), 1.0, 6.0, ((0, 16), (1, 8)))
    input_gate_logits = draw_input_gate_logits(jax.random.fold_in(streams_of[14], 71), 0)
    forget_gate_logits = draw_forget_gate_logits(jax.random.fold_in(streams_of[14], 71), 0)
    extra_forget_logits = draw_extra_forget_logits(jax.random.fold_in(streams_of[14], 71), 0)
    head_norm_gain = jnp.clip(1.0 + 0.18 * jax.random.normal(streams_of[8], (VW,), jnp.float32), 0.099609375, 1.8984375).astype(jnp.bfloat16)
    output_projection_weight = centred(streams_of[9], (VW, D), VW ** -0.5, 0.125, ((0, 8),))
    feedforward_norm_gain = jnp.clip(1.0 + 0.18 * jax.random.normal(streams_of[10], (D,), jnp.float32), 0.099609375, 1.8984375).astype(jnp.bfloat16)
    feedforward_gate_weight = centred(streams_of[11], (D, FF), D ** -0.5, 0.09375, ((0, 16), (1, 8)))
    up_projection_weight = centred(streams_of[12], (D, FF), D ** -0.5, 0.09375, ((0, 16), (1, 8)))
    down_projection_weight = centred(streams_of[13], (D, FF), FF ** -0.5, 0.0546875, ((0, 16), (1, 8)))
    return {"residual": residual, "queries": queries, "projected_key_rows": projected_key_rows, "projected_value_rows": projected_value_rows, "output_gate_logits": output_gate_logits, "input_gate_logits": input_gate_logits, "forget_gate_logits": forget_gate_logits, "extra_forget_logits": extra_forget_logits, "head_norm_gain": head_norm_gain, "output_projection_weight": output_projection_weight, "feedforward_norm_gain": feedforward_norm_gain, "feedforward_gate_weight": feedforward_gate_weight, "up_projection_weight": up_projection_weight, "down_projection_weight": down_projection_weight}


def run_blocks(query_h, key_h, value_h, gate_in, forget_logarithm, state_init, norm_init, peak_init):
    span_len = BLOCK
    blocks_count = query_h.shape[0] // span_len
    query_b = query_h.reshape(blocks_count, span_len, query_h.shape[1])
    key_b = key_h.reshape(blocks_count, span_len, key_h.shape[1])
    value_b = value_h.reshape(blocks_count, span_len, value_h.shape[1])
    gate_b = gate_in.reshape(blocks_count, span_len)
    cum_local = jnp.cumsum(forget_logarithm.reshape(blocks_count, span_len), axis=1)
    cum_last = cum_local[:, -1]
    log_end = cum_last[:, None] - cum_local + gate_b

    def advance(carry, inputs):
        state_now, norm_now, peak_now = carry
        key_blk, value_blk, log_blk, last_blk = inputs
        peak_next = jnp.maximum(last_blk + peak_now, jnp.max(log_blk))
        decay_now = jnp.exp(last_blk + peak_now - peak_next)
        weights = jnp.exp(log_blk - peak_next)
        state_next = decay_now * state_now + jnp.einsum('l,lv,lk->vk', weights, value_blk, key_blk, precision=lax.Precision.HIGHEST)
        norm_next = decay_now * norm_now + jnp.einsum('l,lk->k', weights, key_blk, precision=lax.Precision.HIGHEST)
        return ((state_next, norm_next, peak_next), (state_now, norm_now, peak_now))
    carried, (state_prev, norm_prev, peak_prev) = lax.scan(advance, (state_init, norm_init, peak_init), (key_b, value_b, log_end, cum_last))
    causal = jnp.tril(jnp.ones((span_len, span_len), dtype=bool))
    log_pair = cum_local[:, :, None] - cum_local[:, None, :] + gate_b[:, None, :]
    log_pair = jnp.where(causal[None], log_pair, -jnp.inf)
    inter_log = cum_local + peak_prev[:, None]
    peak_row = jnp.maximum(inter_log, lax.optimization_barrier(jnp.max(log_pair, axis=2)))
    scores = jnp.einsum('cjk,csk->cjs', query_b, key_b, precision=lax.Precision.HIGHEST) * jnp.exp(log_pair - peak_row[:, :, None])
    inter_scale = jnp.exp(inter_log - peak_row)
    numer = jnp.einsum('cjs,csv->cjv', scores, value_b, precision=lax.Precision.HIGHEST)
    numer = numer + inter_scale[:, :, None] * jnp.einsum('cjk,cvk->cjv', query_b, state_prev, precision=lax.Precision.HIGHEST)
    denominator = lax.optimization_barrier(jnp.sum(scores, axis=2)) + inter_scale * jnp.einsum('cjk,ck->cj', query_b, norm_prev, precision=lax.Precision.HIGHEST)
    cell_out = numer / jnp.maximum(jnp.abs(denominator), jnp.exp(-peak_row))[:, :, None]
    return cell_out.reshape(query_h.shape[0], value_h.shape[1])

def by_heads(rows, heads_count):
    tok_count = rows.shape[0]
    return rows.astype(jnp.float32).reshape(tok_count, heads_count, rows.shape[1] // heads_count).transpose(1, 0, 2)

def rms_scaled(values_f32, gain):
    mean_square = lax.optimization_barrier(jnp.mean(values_f32 * values_f32, axis=-1, keepdims=True))
    return values_f32 * lax.rsqrt(mean_square + 1e-06) * gain.astype(jnp.float32)

def reference(residual, queries, projected_key_rows, projected_value_rows, output_gate_logits, input_gate_logits, forget_gate_logits, extra_forget_logits, head_norm_gain, output_projection_weight, feedforward_norm_gain, feedforward_gate_weight, up_projection_weight, down_projection_weight):
    query_h = by_heads(queries, HEADS) * QK_DIM ** (-0.5)
    key_h = by_heads(projected_key_rows, HEADS)
    value_h = by_heads(projected_value_rows, HEADS)
    forget_logarithm = jax.nn.log_sigmoid(forget_gate_logits) + extra_forget_logits
    state_zero = jnp.zeros((HEADS, V_DIM, QK_DIM), jnp.float32)
    norm_zero = jnp.zeros((HEADS, QK_DIM), jnp.float32)
    peak_zero = jnp.zeros((HEADS,), jnp.float32)
    cell_out = jax.vmap(run_blocks)(query_h, key_h, value_h, input_gate_logits, forget_logarithm, state_zero, norm_zero, peak_zero)
    normed_heads = rms_scaled(cell_out, head_norm_gain.reshape(HEADS, 1, V_DIM))
    gated = (normed_heads.transpose(1, 0, 2).reshape(TOKENS, VW) * jax.nn.sigmoid(output_gate_logits.astype(jnp.float32))).astype(jnp.bfloat16)
    group_cols = VW // N_TP
    attn_sum = jnp.zeros((TOKENS, D), jnp.float32)
    for group in range(N_TP):
        partial_out = jnp.dot(gated[:, group * group_cols:(group + 1) * group_cols], output_projection_weight[group * group_cols:(group + 1) * group_cols], preferred_element_type=jnp.float32).astype(jnp.bfloat16)
        attn_sum = attn_sum + lax.optimization_barrier(partial_out).astype(jnp.float32)
    stream = residual.astype(jnp.float32) + attn_sum
    normed = rms_scaled(stream, feedforward_norm_gain).astype(jnp.bfloat16)
    gate_pre = jnp.dot(normed, feedforward_gate_weight, preferred_element_type=jnp.float32)
    up_pre = jnp.dot(normed, up_projection_weight, preferred_element_type=jnp.float32)
    hidden = (jax.nn.silu(gate_pre) * up_pre).astype(jnp.bfloat16)
    hidden_cols = FF // N_TP
    ffn_sum = jnp.zeros((TOKENS, D), jnp.float32)
    for group in range(N_TP):
        partial_ffn = lax.dot_general(hidden[:, group * hidden_cols:(group + 1) * hidden_cols], down_projection_weight[:, group * hidden_cols:(group + 1) * hidden_cols], (((1,), (1,)), ((), ())), preferred_element_type=jnp.float32).astype(jnp.bfloat16)
        ffn_sum = ffn_sum + lax.optimization_barrier(partial_ffn).astype(jnp.float32)
    return (stream + 0.5 * ffn_sum).astype(jnp.bfloat16)
```

```python
import functools

import jax
import jax.numpy as jnp
from jax import lax
from jax.experimental import pallas as pl
from jax.experimental.pallas import tpu as pltpu
from jax.sharding import PartitionSpec as P

MESH = pl.DeviceIdType.MESH
F32 = jnp.float32
BF16 = jnp.bfloat16
HI = lax.Precision.HIGHEST

TOK = 512
D = 4096
MAIN = 640
PADDED = 768
WIDE = 1408
ROWS = 64
CH = 512
SPLIT = {"gu": 176, "d": 128}
NSEM = 256


def nt(a, b, **kw):
    return lax.dot_general(a, b, (((1,), (1,)), ((), ())), preferred_element_type=F32, **kw)


def mm(a, b, **kw):
    return jnp.dot(a, b, preferred_element_type=F32, **kw)


def kernel(
    q_ref, k_ref, v_ref, og_ref, ig_ref, fl_ref, ef_ref, hg_ref, fgain_ref, wout_hbm, res_hbm, gate_hbm, up_hbm,
    down_hbm, out_ref,
    gu_w, d_w, gu_o, d_o, gu_b, d_b, tails, wout, res, nrm, pre, hid, part, a_d2d, a_r1, a_r2, stream, gated,
    f_d2d, f_sum, f_r1, f_r2, f_xr, x_state, x_rows, z_state, z_rows, num_s, row_s, l8,
    ssem, rsem, st_s, st_r, lsem,
):
    sp = lax.axis_index("sp")
    tp = lax.axis_index("tp")
    z, x = sp // 4, sp % 4
    y, c = tp // 2, tp % 2
    h = x % 2
    xp = x + 1 - 2 * h
    xq, xo = (x + 3 + 2 * h) % 4, (x + 2) % 4
    zl, zr, zo = (z + 3) % 4, (z + 1) % 4, (z + 2) % 4
    yl, yr, yo = (y + 3) % 4, (y + 1) % 4, (y + 2) % 4
    oc = 1 - c

    def at(zz, xx, yy, cc):
        return (zz * 4 + xx, yy * 2 + cc)

    core = at(z, x, y, oc)
    x_pair = at(z, xp, y, c)
    y_left, y_right = at(z, x, yl, c), at(z, x, yr, c)
    z_left, z_right = at(zl, x, y, c), at(zr, x, y, c)

    numbers = {}
    pending = {}

    def number(key):
        n = numbers.setdefault(key, len(numbers))
        assert n < NSEM
        return n

    def send(key, src, dst, dev):
        n = number(key)
        d = pltpu.make_async_remote_copy(
            src_ref=src, dst_ref=dst, send_sem=ssem.at[n], recv_sem=rsem.at[n], device_id=dev, device_id_type=MESH
        )
        d.start()
        pending[key] = d

    def arrived(key, ref):
        n = number(key)
        pltpu.make_async_remote_copy(
            src_ref=ref, dst_ref=ref, send_sem=ssem.at[n], recv_sem=rsem.at[n], device_id=core, device_id_type=MESH
        ).wait_recv()

    def sent(key):
        pending.pop(key).wait_send()

    def drain(*heads):
        for key in [k for k in pending if any(k[: len(h)] == h for h in heads)]:
            sent(key)

    barrier = pltpu.get_barrier_semaphore()
    x_others = {"p": at(z, xp, y, c), "q": at(z, xq, y, c), "o": at(z, xo, y, c)}
    z_others = [at(zz, x, y, c) for zz in (zl, zr, zo)]
    for dev in list(x_others.values()) + z_others + [y_left, y_right, core]:
        pl.semaphore_signal(barrier, inc=1, device_id=dev, device_id_type=MESH)

    def local(n, src, dst):
        return pltpu.make_async_copy(src, dst, lsem.at[n])

    own = sp
    oh = 1 - h
    keep = pl.ds(pl.multiple_of(h * MAIN, 128), MAIN)
    give = pl.ds(pl.multiple_of(oh * MAIN, 128), MAIN)
    last = pl.ds(2 * MAIN, 128)
    loads = [
        local(0, gate_hbm.at[:, last], tails.at[0]),
        local(1, up_hbm.at[:, last], tails.at[1]),
        local(2, gate_hbm.at[:, keep], gu_w.at[own, :, 0:MAIN]),
        local(3, up_hbm.at[:, keep], gu_w.at[own, :, PADDED:WIDE]),
        local(4, gate_hbm.at[:, give], gu_o.at[:, 0:MAIN]),
        local(5, up_hbm.at[:, give], gu_o.at[:, PADDED:WIDE]),
        local(6, down_hbm.at[:, keep], d_w.at[own, :, 0:MAIN]),
        local(7, down_hbm.at[:, last], d_w.at[own, :, MAIN:PADDED]),
        local(8, down_hbm.at[:, give], d_o.at[:, 0:MAIN]),
        local(9, down_hbm.at[:, last], d_o.at[:, MAIN:PADDED]),
    ]
    local_wout = local(10, wout_hbm, wout)
    local_res = local(11, res_hbm.at[pl.ds(tp * ROWS, ROWS)], res)
    for d in loads + [local_wout, local_res]:
        d.start()

    l8[...] = jnp.zeros_like(l8)
    fl = fl_ref[...]
    l8[0:2, :] = jnp.minimum(fl, 0.0) - jnp.log1p(jnp.exp(-jnp.abs(fl))) + ef_ref[...]
    logf = l8[...]
    i0 = lax.broadcasted_iota(jnp.int32, (TOK, TOK), 0)
    i1 = lax.broadcasted_iota(jnp.int32, (TOK, TOK), 1)
    cum_row = mm(logf, (i0 <= i1).astype(F32), precision=HI)
    cum_col = nt((i0 >= i1).astype(F32), logf, precision=HI)
    lane = lax.broadcasted_iota(jnp.int32, (1, 128), 1)
    row = lax.broadcasted_iota(jnp.int32, (128, 1), 0)
    a_row, total, w_row, peak = [], [], [], []
    for j in range(2):
        cr = cum_row[j : j + 1, :]
        a = ig_ref[j : j + 1, :] - cr
        t = cr[:, TOK - 1 : TOK]
        log_shard = t + a
        pk = jnp.max(log_shard, axis=1, keepdims=True)
        a_row.append(a)
        total.append(t)
        peak.append(pk)
        w_row.append(jnp.exp(log_shard - pk))
    k = k_ref[...]
    k_t = k.astype(F32).T
    k_tw = (k_t * jnp.where(row < 64, w_row[0], w_row[1])).astype(BF16)
    x_state[x] = jnp.where(row < 64, mm(k_tw, v_ref[:, 0:128]), mm(k_tw, v_ref[:, 128:256])).astype(BF16)
    norms = [mm(jnp.broadcast_to(w_row[j], (16, TOK)).astype(BF16), k)[0:1, :] for j in range(2)]
    x_rows[x, 0:1, :] = jnp.where(lane < 64, norms[0], norms[1])
    x_rows[x, 1:2, :] = jnp.where(lane < 64, total[0], total[1])
    x_rows[x, 2:3, :] = jnp.where(lane < 64, peak[0], peak[1])
    x_rows[x, 3:8, :] = jnp.zeros((5, 128), F32)

    loads[0].wait()
    loads[1].wait()
    gate_tail = tails[0].astype(F32)
    up_tail = pltpu.roll(tails[1].astype(F32), 64, 1)
    low = lane < 64
    mixed = [jnp.where(low, gate_tail, up_tail).astype(BF16), jnp.where(low, up_tail, gate_tail).astype(BF16)]
    gu_w[own, :, MAIN:PADDED] = jnp.where(h == 0, mixed[0], mixed[1])
    gu_o[:, MAIN:PADDED] = jnp.where(h == 0, mixed[1], mixed[0])
    for d in loads[2:]:
        d.wait()

    pl.semaphore_wait(barrier, 9)

    for name, dev in x_others.items():
        send(("xs", name), x_state.at[x], x_state.at[x], dev)
        send(("xt", name), x_rows.at[x], x_rows.at[x], dev)

    def joined(items):
        zero = jnp.zeros((1, 128), F32)
        total_all, tops = zero, []
        for there, _, total_e, peak_e, _ in reversed(items):
            tops.insert(0, jnp.where(there, total_all + peak_e, -1e30))
            total_all = total_all + jnp.where(there, total_e, 0.0)
        peak_all = functools.reduce(jnp.maximum, tops)
        norm, state = zero, jnp.zeros((128, 128), F32)
        for top, (there, norm_e, _, _, state_e) in zip(tops, items):
            w = jnp.exp(top - peak_all)
            norm = norm + jnp.where(there, w * norm_e, 0.0)
            wc = jnp.where(row < 64, w[:, 0:1], w[:, 64:65])
            state = state + jnp.where(there, wc * state_e.astype(F32), 0.0)
        return norm, total_all, peak_all, state

    def item(there, state_ref, rows_ref, e):
        return there, rows_ref[e, 0:1, :], rows_ref[e, 1:2, :], rows_ref[e, 2:3, :], state_ref[e]

    def z_state_copies(s):
        return [
            pltpu.make_async_remote_copy(
                src_ref=ref.at[3], dst_ref=ref.at[jnp.minimum(z, 2)], send_sem=st_s.at[n, s], recv_sem=st_r.at[n, jnp.minimum(z, 2)],
                device_id=at((z + s) % 4, x, y, c), device_id_type=MESH,
            )
            for n, ref in enumerate((z_state, z_rows))
        ]

    room = {"gu": gu_w, "d": d_w}
    other = {"gu": gu_o, "d": d_o}
    stage = {"gu": gu_b, "d": d_b}
    places = {"p": xp, "q": xq, "o": xo}
    turns = {"l": zl, "r": zr, "o": zo}
    sides = {"l": 0, "r": 1, "o": 2}

    def slot(mat, zz, xx, lo=0, hi=256):
        return room[mat].at[zz * 4 + xx, lo:hi]

    def x_own(mat, *names):
        for name in names:
            src = slot(mat, z, x) if name == "o" else other[mat]
            send(("x", mat, name), src, slot(mat, z, x), x_others[name])

    def cut(n):
        return (n // 2 + 15) // 16 * 16

    def z_own(mat):
        for side, dev in (("l", z_right), ("r", z_left)):
            send(("z", mat, "s", side), slot(mat, z, x), slot(mat, z, x), dev)

    def z_other(mat):
        for side, dev in (("l", z_right), ("r", z_left)):
            send(("zb", mat, side), other[mat].at[SPLIT[mat] : 256], stage[mat].at[sides[side]], dev)

    def z_own_forward(mat):
        arrived(("z", mat, "s", "l"), slot(mat, zl, x))
        send(("f", mat, "s", "l"), slot(mat, zl, x, 0, 128), slot(mat, zl, x, 0, 128), z_right)
        arrived(("z", mat, "s", "r"), slot(mat, zr, x))
        send(("f", mat, "s", "r"), slot(mat, zr, x, 128, 256), slot(mat, zr, x, 128, 256), z_left)

    def z_other_forward(mat):
        n = cut(256 - SPLIT[mat])
        arrived(("zb", mat, "l"), stage[mat].at[0])
        send(("fb", mat, "l"), stage[mat].at[0, 0:n], stage[mat].at[2, 0:n], z_right)
        arrived(("zb", mat, "r"), stage[mat].at[1])
        send(("fb", mat, "r"), stage[mat].at[1, n:], stage[mat].at[2, n:], z_left)

    def z_pass(mat, which):
        xx = places[which]
        arrived(("x", mat, which), slot(mat, z, xx))
        for side, dev in (("l", z_right), ("r", z_left)):
            send(("z", mat, which, side), slot(mat, z, xx, 0, SPLIT[mat]), slot(mat, z, xx, 0, SPLIT[mat]), dev)

    def z_pass_forward(mat, which):
        xx, end = places[which], SPLIT[mat]
        n = cut(end)
        arrived(("z", mat, which, "l"), slot(mat, zl, xx, 0, end))
        send(("f", mat, which, "l"), slot(mat, zl, xx, 0, n), slot(mat, zl, xx, 0, n), z_right)
        arrived(("z", mat, which, "r"), slot(mat, zr, xx, 0, end))
        send(("f", mat, which, "r"), slot(mat, zr, xx, n, end), slot(mat, zr, xx, n, end), z_left)

    def x_pass(mat, turn, *names):
        dst = slot(mat, turns[turn], x, SPLIT[mat], 256)
        for name in names:
            src = dst if name == "o" else stage[mat].at[sides[turn]]
            send(("xb", mat, turn, name), src, dst, x_others[name])

    def z_far_own(mat):
        arrived(("f", mat, "s", "l"), slot(mat, zo, x, 0, 128))
        arrived(("f", mat, "s", "r"), slot(mat, zo, x, 128, 256))

    def z_far_other(mat):
        n = cut(256 - SPLIT[mat])
        arrived(("fb", mat, "l"), stage[mat].at[2, 0:n])
        arrived(("fb", mat, "r"), stage[mat].at[2, n:])

    def x_done(mat, turn, *names):
        for which in names:
            arrived(("xb", mat, turn, which), slot(mat, turns[turn], places[which], SPLIT[mat], 256))

    def z_done(mat, *names):
        n = cut(SPLIT[mat])
        for which in names:
            arrived(("f", mat, which, "l"), slot(mat, zo, places[which], 0, n))
            arrived(("f", mat, which, "r"), slot(mat, zo, places[which], n, SPLIT[mat]))

    z_other("gu")
    x_own("gu", "p", "q", "o")
    for name, xx in places.items():
        arrived(("xs", name), x_state.at[xx])
        arrived(("xt", name), x_rows.at[xx])
    norm, total_all, peak_all, state = joined([item(True, x_state, x_rows, e) for e in range(4)])
    z_state[3] = state.astype(BF16)
    z_rows[3, 0:1, :] = norm
    z_rows[3, 1:2, :] = total_all
    z_rows[3, 2:3, :] = peak_all
    z_rows[3, 3:8, :] = jnp.zeros((5, 128), F32)
    for s in range(1, 4):
        @pl.when(z + s < 4)
        def _():
            for d in z_state_copies(s):
                d.start()
    z_own("gu")
    z_other("d")

    q8 = q_ref[...] * jnp.asarray(0.125, BF16)
    q_h = [jnp.where((lane < 64) == (j == 0), q8, jnp.zeros_like(q8)) for j in range(2)]
    for j in range(2):
        for r in range(4):
            n = (r + 1) * 128
            rows = slice(r * 128, n)
            s = nt(q_h[j][rows, :], k_ref[0:n, :])
            lp = cum_col[rows, j : j + 1] + a_row[j][:, 0:n]
            ti = lax.broadcasted_iota(jnp.int32, (128, n), 0) + r * 128
            si = lax.broadcasted_iota(jnp.int32, (128, n), 1)
            lp = jnp.where(si <= ti, lp, -jnp.inf)
            m = jnp.max(lp, axis=1, keepdims=True)
            p = s * jnp.exp(lp - m)
            row_s[j, rows, 0:1] = m
            row_s[j, rows, 1:2] = jnp.sum(p, axis=1, keepdims=True)
            num_s[j, rows, :] = mm(p.astype(BF16), v_ref[0:n, j * 128 : (j + 1) * 128])

    for e in range(3):
        @pl.when(e < z)
        def _():
            for n, ref in enumerate((z_state, z_rows)):
                pltpu.make_async_remote_copy(
                    src_ref=ref.at[e], dst_ref=ref.at[e], send_sem=st_s.at[n, 0], recv_sem=st_r.at[n, e],
                    device_id=core, device_id_type=MESH,
                ).wait_recv()

    norm, total_all, peak_all, state = joined(
        [item(e < z, z_state, z_rows, e) for e in range(3)] + [item(e < x, x_state, x_rows, e) for e in range(3)]
    )
    peak_in = jnp.maximum(peak_all, total_all)
    rescale = jnp.exp(peak_all - peak_in)
    norm = norm * rescale
    state = (state * jnp.where(row < 64, rescale[:, 0:1], rescale[:, 64:65])).astype(BF16)
    for j in range(2):
        il = cum_col[:, j : j + 1] + peak_in[:, 64 * j : 64 * j + 1]
        m = row_s[j, :, 0:1]
        pr = jnp.maximum(il, m)
        e1, e2 = jnp.exp(m - pr), jnp.exp(il - pr)
        numer = e1 * num_s[j] + e2 * mm(q_h[j], state)
        denom = e1 * row_s[j, :, 1:2] + e2 * jnp.sum(q_h[j].astype(F32) * norm, axis=1, keepdims=True)
        cell = numer / jnp.maximum(jnp.abs(denom), jnp.exp(-pr))
        mean = jnp.mean(cell * cell, axis=1, keepdims=True)
        cols = slice(j * 128, (j + 1) * 128)
        g = cell * lax.rsqrt(mean + 1e-06) * hg_ref[cols].astype(F32)[None, :] * jax.nn.sigmoid(og_ref[:, cols].astype(F32))
        gated[:, cols] = g.astype(BF16)

    local_wout.wait()
    local_res.wait()
    def cols_of(i):
        return slice(i * CH, (i + 1) * CH)

    for i in range(4):
        for n in range(2):
            r = mm(gated[...], wout[:, cols_of(2 * i + n)]).astype(BF16)
            part[i, :, n] = r.reshape(4, 2, ROWS, CH)
        send(("ad", i), part.at[i, :, :, oc], a_d2d.at[i], core)
    for i in range(4):
        arrived(("ad", i), a_d2d.at[i])
        f_sum[4 + i] = (part[i, :, :, c].astype(F32) + a_d2d[i].astype(F32)).astype(BF16)
        send(("a1l", i), f_sum.at[4 + i, yo, :, 0:32], a_r1.at[i, 0], y_right)
        send(("a1r", i), f_sum.at[4 + i, yo, :, 32:64], a_r1.at[i, 1], y_left)
    z_pass("gu", "p")
    for i in range(4):
        arrived(("a1l", i), a_r1.at[i, 0])
        f_sum[4 + i, yr, :, 0:32] = (f_sum[4 + i, yr, :, 0:32].astype(F32) + a_r1[i, 0].astype(F32)).astype(BF16)
        send(("a2l", i), f_sum.at[4 + i, yr], a_r2.at[i, 0], y_right)
        arrived(("a1r", i), a_r1.at[i, 1])
        f_sum[4 + i, yl, :, 32:64] = (f_sum[4 + i, yl, :, 32:64].astype(F32) + a_r1[i, 1].astype(F32)).astype(BF16)
        send(("a2r", i), f_sum.at[4 + i, yl], a_r2.at[i, 1], y_left)
    z_own_forward("gu")
    z_pass("gu", "q")
    square = jnp.zeros((ROWS, 1), F32)
    for i in range(4):
        arrived(("a2l", i), a_r2.at[i, 0])
        arrived(("a2r", i), a_r2.at[i, 1])
        for n in range(2):
            cols = cols_of(2 * i + n)
            s = part[i, y, n, c].astype(F32) + a_d2d[i, y, n].astype(F32)
            s = s + a_r2[i, 0, n].astype(F32) + a_r2[i, 1, n].astype(F32) + res[:, cols].astype(F32)
            stream[:, cols] = s
            square = square + jnp.sum(s * s, axis=1, keepdims=True)
    scale = lax.rsqrt(square * (1.0 / D) + 1e-06)
    for i in range(8):
        cols = cols_of(i)
        nrm[y, h, c, :, cols] = (stream[:, cols] * scale * fgain_ref[cols].astype(F32)[None, :]).astype(BF16)

    def rows_of(yy, pp, cc, half=None):
        ref = nrm.at[yy, pp, cc]
        return ref if half is None else ref.at[half * 32 : (half + 1) * 32]

    def pass_on(key, yy, pp, dev, half=None):
        send(key, rows_of(yy, pp, c, half), rows_of(yy, pp, c, half), dev)

    pass_on(("ny", 0, "l"), y, h, y_right)
    pass_on(("ny", 0, "r"), y, h, y_left)
    pass_on(("nx",), y, h, x_pair)
    pass_on(("nc", 0, 0), y, h, core)
    z_other_forward("gu")
    for turn in ("l", "r"):
        x_pass("gu", turn, "p", "q", "o")
    x_own("d", "p", "q")
    z_pass("gu", "o")
    for s in range(1, 4):
        @pl.when(z + s < 4)
        def _():
            for d in z_state_copies(s):
                d.wait_send()
    drain(("xs",), ("xt",), ("ad",), ("a1l",), ("a1r",), ("a2l",), ("a2r",), ("zb", "gu"), ("z", "gu", "s"), ("x", "gu"))
    arrived(("nx",), rows_of(y, oh, c))
    pass_on(("ny", 1, "l"), y, oh, y_right)
    pass_on(("ny", 1, "r"), y, oh, y_left)
    pass_on(("nc", 0, 1), y, oh, core)

    def ring_forward(n, pp):
        arrived(("ny", n, "l"), rows_of(yl, pp, c))
        pass_on(("nf", n, "l"), yl, pp, y_right, 0)
        pass_on(("nc", 1, n), yl, pp, core)
        arrived(("ny", n, "r"), rows_of(yr, pp, c))
        pass_on(("nf", n, "r"), yr, pp, y_left, 1)
        pass_on(("nc", 2, n), yr, pp, core)

    def ring_last(n, pp):
        arrived(("nf", n, "l"), rows_of(yo, pp, c, 0))
        arrived(("nf", n, "r"), rows_of(yo, pp, c, 1))
        pass_on(("nc", 3, n), yo, pp, core)

    def from_core(place, yy):
        arrived(("nc", place, 0), rows_of(yy, h, oc))
        arrived(("nc", place, 1), rows_of(yy, oh, oc))

    def gu_tile(yy, kz, first):
        xs = nrm[yy, :, :, :, pl.ds(pl.multiple_of(kz * 1024, 1024), 1024)].reshape(256, 1024)
        for lo, hi in ((0, 512), (512, 1024), (1024, 1408)):
            r = mm(xs, gu_w[pl.ds(kz * 4, 4), :, lo:hi].reshape(1024, hi - lo))
            pre[yy, :, lo:hi] = r if first else pre[yy, :, lo:hi] + r

    def nth(base, i):
        return (base + i + i // 2 - 2 * (i // 3)) % 4

    ring_forward(0, h)
    z_pass_forward("gu", "p")
    from_core(0, y)
    gu_tile(y, z, True)
    drain(("zb",), ("nx",), ("ny", 0), ("nc", 0), ("z", "gu", "p"), ("f", "gu", "s"))
    z_pass_forward("gu", "q")
    z_far_own("gu")
    z_far_other("gu")
    x_pass("gu", "o", "p", "q", "o")
    x_own("d", "o")
    z_other_forward("d")
    for turn in ("l", "r"):
        x_pass("d", turn, "p", "q")
    ring_forward(1, oh)
    from_core(1, yl)
    from_core(2, yr)

    @pl.loop(0, 2)
    def _(i):
        gu_tile((y + 1 + 2 * i) % 4, z, True)

    ring_last(0, h)
    z_pass_forward("gu", "o")
    z_own("d")
    z_pass("d", "p")
    z_pass("d", "q")
    x_done("gu", "l", "p", "q", "o")

    @pl.loop(0, 3)
    def _(i):
        gu_tile((y + i + i // 2) % 4, zl, False)

    ring_last(1, oh)
    x_done("gu", "r", "p", "q", "o")

    @pl.loop(0, 3)
    def _(i):
        gu_tile((y + i + i // 2) % 4, zr, False)

    from_core(3, yo)
    gu_tile(yo, z, True)

    @pl.loop(0, 2)
    def _(i):
        gu_tile(yo, (z + 1 + 2 * i) % 4, False)

    drain(("ny",), ("nf",), ("nc",), ("z", "gu"), ("fb",), ("x", "d", "p"), ("x", "d", "q"), ("xb", "gu"))
    drain(("f", "gu", "p"), ("f", "gu", "q"))
    z_done("gu", "p", "q")
    x_done("gu", "o", "p", "q", "o")

    def gu_slot(yy, zz, xx):
        k = zz * 4 + xx
        xs = nrm[yy, :, :, :, pl.ds(pl.multiple_of(k * 256, 256), 256)].reshape(256, 256)
        for lo, hi in ((0, 512), (512, 1024), (1024, 1408)):
            pre[yy, :, lo:hi] += mm(xs, gu_w[k, :, lo:hi])

    @pl.loop(0, 4)
    def _(yy):
        for xx in (x, xp, xq):
            gu_slot(yy, zo, xx)

    z_done("gu", "o")

    @pl.loop(0, 4)
    def _(yy):
        gu_slot(yy, zo, xo)
        rows = pl.ds(pl.multiple_of(yy * 256, 256), 256)
        hid[rows, 0:MAIN] = (jax.nn.silu(pre[yy, :, 0:MAIN]) * pre[yy, :, PADDED:WIDE]).astype(BF16)
        tail = pre[yy, :, MAIN:PADDED]
        both = jax.nn.silu(tail) * pltpu.roll(tail, 64, 1)
        hid[rows, MAIN:PADDED] = jnp.where(low == (h == 0), both, 0.0).astype(BF16)

    near, away = x // 2, 1 - x // 2
    order = [(z, near), (z, away), (zl, near), (zr, near), (zl, away), (zr, away), (zo, near), (zo, away)]

    def down(i):
        zz, j = order[i]
        if i >= 4:
            sent(("fd", i - 4))

        @pl.loop(0, 2)
        def _(s):
            r = nt(hid[...], d_w[zz * 4 + j * 2 + s]).astype(BF16)
            part[i % 4, :, :, :, :, pl.ds(pl.multiple_of(s * 256, 256), 256)] = r.reshape(4, 2, 2, ROWS, 256)

        send(("fd", i), part.at[i % 4, :, :, oc], f_d2d.at[i], core)

    def sum_cores(i):
        arrived(("fd", i), f_d2d.at[i])
        f_sum[i] = (part[i % 4, :, :, c].astype(F32) + f_d2d[i].astype(F32)).astype(BF16)
        send(("f1l", i), f_sum.at[i, yo, :, 0:32], f_r1.at[i, 0], y_right)
        send(("f1r", i), f_sum.at[i, yo, :, 32:64], f_r1.at[i, 1], y_left)

    def sum_far(i):
        arrived(("f1l", i), f_r1.at[i, 0])
        f_sum[i, yr, :, 0:32] = (f_sum[i, yr, :, 0:32].astype(F32) + f_r1[i, 0].astype(F32)).astype(BF16)
        send(("f2l", i), f_sum.at[i, yr], f_r2.at[i, 0], y_right)
        arrived(("f1r", i), f_r1.at[i, 1])
        f_sum[i, yl, :, 32:64] = (f_sum[i, yl, :, 32:64].astype(F32) + f_r1[i, 1].astype(F32)).astype(BF16)
        send(("f2r", i), f_sum.at[i, yl], f_r2.at[i, 1], y_left)

    def ring_sum(i, pp):
        return f_sum[i, y, pp].astype(F32) + f_r2[i, 0, pp].astype(F32) + f_r2[i, 1, pp].astype(F32)

    def sum_near(i):
        if i >= 2:
            drain(("f1l", i - 1), ("f1r", i - 1), ("f2l", i - 2), ("f2r", i - 2), ("fx", i - 2))
        arrived(("f2l", i), f_r2.at[i, 0])
        arrived(("f2r", i), f_r2.at[i, 1])
        f_sum[i, y, oh] = ring_sum(i, oh).astype(BF16)
        send(("fx", i), f_sum.at[i, y, oh], f_xr.at[i], x_pair)

    def finish(i):
        zz, j = order[i]
        arrived(("fx", i), f_xr.at[i])
        cols = pl.ds(pl.multiple_of(zz * 1024 + j * CH, CH), CH)
        out_ref[:, cols] = (stream[:, cols] + 0.5 * (ring_sum(i, h) + f_xr[i].astype(F32))).astype(BF16)

    down(0)
    z_pass("d", "o")
    down(1)
    sum_cores(0)
    z_own_forward("d")
    for turn in ("l", "r"):
        x_pass("d", turn, "o")
    z_far_other("d")
    x_pass("d", "o", "p", "q")
    sum_cores(1)
    sum_far(0)
    z_pass_forward("d", "p")
    x_done("d", "l", "p")
    down(2)
    x_done("d", "r", "p")
    down(3)
    sum_far(1)
    sum_cores(2)
    sum_near(0)
    sum_cores(3)
    z_pass_forward("d", "q")
    sum_near(1)
    sum_far(2)
    z_pass_forward("d", "o")
    x_done("d", "l", "q", "o")
    down(4)
    x_done("d", "r", "q", "o")
    down(5)
    sum_far(3)
    z_far_own("d")
    x_pass("d", "o", "o")
    sum_cores(4)
    sum_cores(5)
    sum_near(2)
    drain(("x", "d"), ("z", "d"), ("f", "gu"), ("xb", "d", "l"), ("xb", "d", "r"), ("f", "d", "s"))
    z_done("d", "p")
    x_done("d", "o", "p")
    down(6)
    sum_far(4)
    sum_near(3)
    sum_cores(6)
    z_done("d", "q", "o")
    x_done("d", "o", "q", "o")
    down(7)
    sum_far(5)
    sum_near(4)
    sum_cores(7)
    finish(0)
    sum_far(6)
    finish(1)
    sum_near(5)
    finish(2)
    sum_far(7)
    for i in range(3, 6):
        finish(i)
    sum_near(6)
    sum_near(7)
    finish(6)
    drain(("f",), ("xb",), ("fd",))
    finish(7)

    for key in list(pending):
        sent(key)


def per_device(
    residual, queries, keys, values, output_gate, input_gate, forget_gate, extra_forget, head_gain, wout, ffn_gain,
    gate_w, up_w, down_w,
):
    vmem = pl.BlockSpec(memory_space=pltpu.VMEM)
    anywhere = pl.BlockSpec(memory_space=pl.ANY)
    scratch = [
        pltpu.VMEM((16, 256, WIDE), BF16),
        pltpu.VMEM((16, 256, PADDED), BF16),
        pltpu.VMEM((256, WIDE), BF16),
        pltpu.VMEM((256, PADDED), BF16),
        pltpu.VMEM((3, 256 - SPLIT["gu"], WIDE), BF16),
        pltpu.VMEM((3, 256 - SPLIT["d"], PADDED), BF16),
        pltpu.VMEM((2, 256, 128), BF16),
        pltpu.VMEM((256, D), BF16),
        pltpu.VMEM((ROWS, D), BF16),
        pltpu.VMEM((4, 2, 2, ROWS, D), BF16),
        pltpu.VMEM((4, 256, WIDE), F32),
        pltpu.VMEM((1024, PADDED), BF16),
        pltpu.VMEM((4, 4, 2, 2, ROWS, CH), BF16),
        pltpu.VMEM((4, 4, 2, ROWS, CH), BF16),
        pltpu.VMEM((4, 2, 2, 32, CH), BF16),
        pltpu.VMEM((4, 2, 2, ROWS, CH), BF16),
        pltpu.VMEM((ROWS, D), F32),
        pltpu.VMEM((TOK, 256), BF16),
        pltpu.VMEM((8, 4, 2, ROWS, CH), BF16),
        pltpu.VMEM((8, 4, 2, ROWS, CH), BF16),
        pltpu.VMEM((8, 2, 2, 32, CH), BF16),
        pltpu.VMEM((8, 2, 2, ROWS, CH), BF16),
        pltpu.VMEM((8, ROWS, CH), BF16),
        pltpu.VMEM((4, 128, 128), BF16),
        pltpu.VMEM((4, 8, 128), F32),
        pltpu.VMEM((4, 128, 128), BF16),
        pltpu.VMEM((4, 8, 128), F32),
        pltpu.VMEM((2, TOK, 128), F32),
        pltpu.VMEM((2, TOK, 2), F32),
        pltpu.VMEM((8, TOK), F32),
        pltpu.SemaphoreType.DMA((NSEM,)),
        pltpu.SemaphoreType.DMA((NSEM,)),
        pltpu.SemaphoreType.DMA((2, 4)),
        pltpu.SemaphoreType.DMA((2, 4)),
        pltpu.SemaphoreType.DMA((12,)),
    ]
    return pl.pallas_call(
        kernel,
        out_shape=jax.ShapeDtypeStruct((ROWS, D), BF16),
        in_specs=[vmem] * 9 + [anywhere] * 5,
        out_specs=vmem,
        scratch_shapes=scratch,
        compiler_params=pltpu.CompilerParams(
            collective_id=0, has_side_effects=True, vmem_limit_bytes=67_043_328
        ),
        name="layer",
    )(
        queries, keys, values, output_gate, input_gate, forget_gate, extra_forget,
        head_gain, ffn_gain, wout, residual, gate_w, up_w, down_w,
    )


def solution(mesh):
    tp_sp = P("tp", "sp")
    rows = P("sp", "tp")
    in_specs = (
        P("sp", None), rows, rows, rows, rows, tp_sp, tp_sp, tp_sp, P("tp"), P("tp", None), P(), rows, rows, rows,
    )
    return jax.shard_map(
        per_device, mesh=mesh, in_specs=in_specs, out_specs=P(("sp", "tp"), None), check_vma=False
    )
```

```python
import functools

import jax
import jax.numpy as jnp
from jax import lax
from jax.experimental import pallas as pl
from jax.experimental.pallas import tpu as pltpu
from jax.sharding import PartitionSpec as P

MESH = pl.DeviceIdType.MESH
F32 = jnp.float32
BF16 = jnp.bfloat16
HI = lax.Precision.HIGHEST

TOK = 512
D = 4096
MAIN = 640
PADDED = 768
WIDE = 1408
ROWS = 64
CH = 512
SPLIT = {"gu": 176, "d": 128}
NSEM = 143
NSEND = 58


def nt(a, b, **kw):
    return lax.dot_general(a, b, (((1,), (1,)), ((), ())), preferred_element_type=F32, **kw)


def mm(a, b, **kw):
    return jnp.dot(a, b, preferred_element_type=F32, **kw)


def kernel(
    q_hbm, k_hbm, v_hbm, og_hbm, ig_hbm, fl_hbm, ef_hbm, hg_hbm, fgain_hbm, wout_hbm, res_hbm, gate_hbm, up_hbm,
    down_hbm, out_ref,
    q_ref, k_ref, v_ref, og_ref, ig_ref, fl_ref, ef_ref, hg_ref, fgain_ref,
    gu_w, d_w, gu_o, d_o, gu_b, d_b, tails, wout, res, nrm, pre, hid, part, a_d2d, a_r1, a_r2, stream, gated,
    f_d2d, f_sum, f_r1, f_r2, f_xr, x_state, x_rows, z_state, z_rows, num_s, row_s, l8,
    ssem, rsem, st_s, st_r, lsem,
):
    sp = lax.axis_index("sp")
    tp = lax.axis_index("tp")
    z, x = sp // 4, sp % 4
    y, c = tp // 2, tp % 2
    h = x % 2
    xp = x + 1 - 2 * h
    xq, xo = (x + 3 + 2 * h) % 4, (x + 2) % 4
    zl, zr, zo = (z + 3) % 4, (z + 1) % 4, (z + 2) % 4
    yl, yr, yo = (y + 3) % 4, (y + 1) % 4, (y + 2) % 4
    oc = 1 - c

    def at(zz, xx, yy, cc):
        return (zz * 4 + xx, yy * 2 + cc)

    core = at(z, x, y, oc)
    x_pair = at(z, xp, y, c)
    y_left, y_right = at(z, x, yl, c), at(z, x, yr, c)
    z_left, z_right = at(zl, x, y, c), at(zr, x, y, c)

    numbers = {}
    pending = {}
    free = list(range(NSEND))

    def number(key):
        n = numbers.setdefault(key, len(numbers))
        assert n < NSEM
        return n

    def send(key, src, dst, dev, at_key=None):
        slot_s = free.pop(0)
        d = pltpu.make_async_remote_copy(
            src_ref=src, dst_ref=dst, send_sem=ssem.at[slot_s], recv_sem=rsem.at[number(at_key or key)], device_id=dev,
            device_id_type=MESH,
        )
        d.start()
        pending[key] = d, slot_s

    def arrived(key, ref):
        n = number(key)
        pltpu.make_async_remote_copy(
            src_ref=ref, dst_ref=ref, send_sem=ssem.at[0], recv_sem=rsem.at[n], device_id=core, device_id_type=MESH
        ).wait_recv()

    def sent(key):
        d, slot_s = pending.pop(key)
        d.wait_send()
        free.append(slot_s)

    def drain(*heads):
        for key in [k for k in pending if any(k[: len(h)] == h for h in heads)]:
            sent(key)

    barrier = pltpu.get_barrier_semaphore()
    x_others = {"p": at(z, xp, y, c), "q": at(z, xq, y, c), "o": at(z, xo, y, c)}
    z_others = [at(zz, x, y, c) for zz in (zl, zr, zo)]
    for dev in list(x_others.values()) + z_others + [y_left, y_right, core]:
        pl.semaphore_signal(barrier, inc=1, device_id=dev, device_id_type=MESH)

    def local(n, src, dst):
        return pltpu.make_async_copy(src, dst, lsem.at[n])

    own = sp
    oh = 1 - h
    keep = pl.ds(pl.multiple_of(h * MAIN, 128), MAIN)
    give = pl.ds(pl.multiple_of(oh * MAIN, 128), MAIN)
    last = pl.ds(2 * MAIN, 128)
    loads = [
        local(0, gate_hbm.at[:, last], tails.at[0]),
        local(1, up_hbm.at[:, last], tails.at[1]),
        local(2, gate_hbm.at[:, keep], gu_w.at[own, :, 0:MAIN]),
        local(3, up_hbm.at[:, keep], gu_w.at[own, :, PADDED:WIDE]),
        local(4, gate_hbm.at[:, give], gu_o.at[:, 0:MAIN]),
        local(5, up_hbm.at[:, give], gu_o.at[:, PADDED:WIDE]),
        local(6, down_hbm.at[:, keep], d_w.at[own, :, 0:MAIN]),
        local(7, down_hbm.at[:, last], d_w.at[own, :, MAIN:PADDED]),
        local(8, down_hbm.at[:, give], d_o.at[:, 0:MAIN]),
        local(9, down_hbm.at[:, last], d_o.at[:, MAIN:PADDED]),
    ]
    local_wout = local(10, wout_hbm, wout)
    local_res = local(11, res_hbm.at[pl.ds(tp * ROWS, ROWS)], res)
    first = [
        local(12 + n, src, dst)
        for n, (src, dst) in enumerate(
            (
                (fl_hbm, fl_ref), (ef_hbm, ef_ref), (ig_hbm, ig_ref), (k_hbm, k_ref), (v_hbm, v_ref), (q_hbm, q_ref),
                (og_hbm, og_ref), (hg_hbm, hg_ref), (fgain_hbm, fgain_ref),
            )
        )
    ]
    for d in first + loads + [local_wout, local_res]:
        d.start()
    for d in first[:5]:
        d.wait()

    l8[...] = jnp.zeros_like(l8)
    fl = fl_ref[...]
    l8[0:2, :] = jnp.minimum(fl, 0.0) - jnp.log1p(jnp.exp(-jnp.abs(fl))) + ef_ref[...]
    logf = l8[...]
    i0 = lax.broadcasted_iota(jnp.int32, (TOK, TOK), 0)
    i1 = lax.broadcasted_iota(jnp.int32, (TOK, TOK), 1)
    cum_row = mm(logf, (i0 <= i1).astype(F32), precision=HI)
    cum_col = nt((i0 >= i1).astype(F32), logf, precision=HI)
    lane = lax.broadcasted_iota(jnp.int32, (1, 128), 1)
    row = lax.broadcasted_iota(jnp.int32, (128, 1), 0)
    a_row, total, w_row, peak = [], [], [], []
    for j in range(2):
        cr = cum_row[j : j + 1, :]
        a = ig_ref[j : j + 1, :] - cr
        t = cr[:, TOK - 1 : TOK]
        log_shard = t + a
        pk = jnp.max(log_shard, axis=1, keepdims=True)
        a_row.append(a)
        total.append(t)
        peak.append(pk)
        w_row.append(jnp.exp(log_shard - pk))
    k = k_ref[...]
    k_t = k.astype(F32).T
    k_tw = k_t * jnp.where(row < 64, w_row[0], w_row[1])
    k_hi = k_tw.astype(BF16)
    k_lo = (k_tw - k_hi.astype(F32)).astype(BF16)
    states = [mm(k_hi, v_ref[:, n : n + 128]) + mm(k_lo, v_ref[:, n : n + 128]) for n in (0, 128)]
    x_state[x] = jnp.where(row < 64, states[0], states[1])
    norms = [mm(jnp.broadcast_to(w_row[j], (16, TOK)).astype(BF16), k)[0:1, :] for j in range(2)]
    x_rows[x, 0:1, :] = jnp.where(lane < 64, norms[0], norms[1])
    x_rows[x, 1:2, :] = jnp.where(lane < 64, total[0], total[1])
    x_rows[x, 2:3, :] = jnp.where(lane < 64, peak[0], peak[1])
    x_rows[x, 3:8, :] = jnp.zeros((5, 128), F32)

    loads[0].wait()
    loads[1].wait()
    gate_tail = tails[0].astype(F32)
    up_tail = pltpu.roll(tails[1].astype(F32), 64, 1)
    low = lane < 64
    mixed = [jnp.where(low, gate_tail, up_tail).astype(BF16), jnp.where(low, up_tail, gate_tail).astype(BF16)]
    gu_w[own, :, MAIN:PADDED] = jnp.where(h == 0, mixed[0], mixed[1])
    gu_o[:, MAIN:PADDED] = jnp.where(h == 0, mixed[1], mixed[0])
    for d in loads[2:]:
        d.wait()

    pl.semaphore_wait(barrier, 9)

    for name, dev in x_others.items():
        send(("xs", name), x_state.at[x], x_state.at[x], dev)
        send(("xt", name), x_rows.at[x], x_rows.at[x], dev)

    def joined(items):
        zero = jnp.zeros((1, 128), F32)
        total_all, tops = zero, []
        for there, _, total_e, peak_e, _ in reversed(items):
            tops.insert(0, jnp.where(there, total_all + peak_e, -1e30))
            total_all = total_all + jnp.where(there, total_e, 0.0)
        peak_all = functools.reduce(jnp.maximum, tops)
        norm, state = zero, jnp.zeros((128, 128), F32)
        for top, (there, norm_e, _, _, state_e) in zip(tops, items):
            w = jnp.exp(top - peak_all)
            norm = norm + jnp.where(there, w * norm_e, 0.0)
            wc = jnp.where(row < 64, w[:, 0:1], w[:, 64:65])
            state = state + jnp.where(there, wc * state_e, 0.0)
        return norm, total_all, peak_all, state

    def item(there, state_ref, rows_ref, e):
        return there, rows_ref[e, 0:1, :], rows_ref[e, 1:2, :], rows_ref[e, 2:3, :], state_ref[e]

    def z_state_copies(s):
        return [
            pltpu.make_async_remote_copy(
                src_ref=ref.at[3], dst_ref=ref.at[jnp.minimum(z, 2)], send_sem=st_s.at[n, s], recv_sem=st_r.at[n, jnp.minimum(z, 2)],
                device_id=at((z + s) % 4, x, y, c), device_id_type=MESH,
            )
            for n, ref in enumerate((z_state, z_rows))
        ]

    room = {"gu": gu_w, "d": d_w}
    other = {"gu": gu_o, "d": d_o}
    stage = {"gu": gu_b, "d": d_b}
    places = {"p": xp, "q": xq, "o": xo}
    turns = {"l": zl, "r": zr, "o": zo}
    sides = {"l": 0, "r": 1, "o": 2}

    def slot(mat, zz, xx, lo=0, hi=256):
        return room[mat].at[zz * 4 + xx, lo:hi]

    def x_own(mat, *names):
        for name in names:
            src = slot(mat, z, x) if name == "o" else other[mat]
            send(("x", mat, name), src, slot(mat, z, x), x_others[name])

    def cut(n):
        return (n // 2 + 15) // 16 * 16

    def z_own(mat):
        for side, dev in (("l", z_right), ("r", z_left)):
            send(("z", mat, "s", side), slot(mat, z, x), slot(mat, z, x), dev)

    def z_other(mat):
        for side, dev in (("l", z_right), ("r", z_left)):
            send(("zb", mat, side), other[mat].at[SPLIT[mat] : 256], stage[mat].at[sides[side]], dev)

    def z_own_forward(mat):
        arrived(("z", mat, "s", "l"), slot(mat, zl, x))
        send(("f", mat, "s", "l"), slot(mat, zl, x, 0, 128), slot(mat, zl, x, 0, 128), z_right)
        arrived(("z", mat, "s", "r"), slot(mat, zr, x))
        send(("f", mat, "s", "r"), slot(mat, zr, x, 128, 256), slot(mat, zr, x, 128, 256), z_left)

    def z_other_forward(mat):
        n = cut(256 - SPLIT[mat])
        arrived(("zb", mat, "l"), stage[mat].at[0])
        send(("fb", mat, "l"), stage[mat].at[0, 0:n], stage[mat].at[2, 0:n], z_right)
        arrived(("zb", mat, "r"), stage[mat].at[1])
        send(("fb", mat, "r"), stage[mat].at[1, n:], stage[mat].at[2, n:], z_left)

    def z_pass(mat, which):
        xx = places[which]
        arrived(("x", mat, which), slot(mat, z, xx))
        for side, dev in (("l", z_right), ("r", z_left)):
            send(("z", mat, which, side), slot(mat, z, xx, 0, SPLIT[mat]), slot(mat, z, xx, 0, SPLIT[mat]), dev)

    def z_pass_forward(mat, which):
        xx, end = places[which], SPLIT[mat]
        n = cut(end)
        arrived(("z", mat, which, "l"), slot(mat, zl, xx, 0, end))
        send(("f", mat, which, "l"), slot(mat, zl, xx, 0, n), slot(mat, zl, xx, 0, n), z_right)
        arrived(("z", mat, which, "r"), slot(mat, zr, xx, 0, end))
        send(("f", mat, which, "r"), slot(mat, zr, xx, n, end), slot(mat, zr, xx, n, end), z_left)

    def x_pass(mat, turn, *names):
        dst = slot(mat, turns[turn], x, SPLIT[mat], 256)
        for name in names:
            src = dst if name == "o" else stage[mat].at[sides[turn]]
            send(("xb", mat, turn, name), src, dst, x_others[name])

    def z_far_own(mat):
        arrived(("f", mat, "s", "l"), slot(mat, zo, x, 0, 128))
        arrived(("f", mat, "s", "r"), slot(mat, zo, x, 128, 256))

    def z_far_other(mat):
        n = cut(256 - SPLIT[mat])
        arrived(("fb", mat, "l"), stage[mat].at[2, 0:n])
        arrived(("fb", mat, "r"), stage[mat].at[2, n:])

    def x_done(mat, turn, *names):
        for which in names:
            arrived(("xb", mat, turn, which), slot(mat, turns[turn], places[which], SPLIT[mat], 256))

    def z_done(mat, *names):
        n = cut(SPLIT[mat])
        for which in names:
            arrived(("f", mat, which, "l"), slot(mat, zo, places[which], 0, n))
            arrived(("f", mat, which, "r"), slot(mat, zo, places[which], n, SPLIT[mat]))

    z_other("gu")
    x_own("gu", "p", "q", "o")
    for name, xx in places.items():
        arrived(("xs", name), x_state.at[xx])
        arrived(("xt", name), x_rows.at[xx])
    norm, total_all, peak_all, state = joined([item(True, x_state, x_rows, e) for e in range(4)])
    z_state[3] = state
    z_rows[3, 0:1, :] = norm
    z_rows[3, 1:2, :] = total_all
    z_rows[3, 2:3, :] = peak_all
    z_rows[3, 3:8, :] = jnp.zeros((5, 128), F32)
    for s in range(1, 4):
        @pl.when(z + s < 4)
        def _():
            for d in z_state_copies(s):
                d.start()
    z_own("gu")

    for d in first[5:]:
        d.wait()
    q8 = q_ref[...] * jnp.asarray(0.125, BF16)
    q_h = [jnp.where((lane < 64) == (j == 0), q8, jnp.zeros_like(q8)) for j in range(2)]
    for j in range(2):
        for r in range(4):
            n = (r + 1) * 128
            rows = slice(r * 128, n)
            s = nt(q_h[j][rows, :], k_ref[0:n, :])
            lp = cum_col[rows, j : j + 1] + a_row[j][:, 0:n]
            ti = lax.broadcasted_iota(jnp.int32, (128, n), 0) + r * 128
            si = lax.broadcasted_iota(jnp.int32, (128, n), 1)
            lp = jnp.where(si <= ti, lp, -jnp.inf)
            m = jnp.max(lp, axis=1, keepdims=True)
            p = s * jnp.exp(lp - m)
            row_s[j, rows, 0:1] = m
            row_s[j, rows, 1:2] = jnp.sum(p, axis=1, keepdims=True)
            num_s[j, rows, :] = mm(p.astype(BF16), v_ref[0:n, j * 128 : (j + 1) * 128])

    for e in range(3):
        @pl.when(e < z)
        def _():
            for n, ref in enumerate((z_state, z_rows)):
                pltpu.make_async_remote_copy(
                    src_ref=ref.at[e], dst_ref=ref.at[e], send_sem=st_s.at[n, 0], recv_sem=st_r.at[n, e],
                    device_id=core, device_id_type=MESH,
                ).wait_recv()

    norm, total_all, peak_all, state = joined(
        [item(e < z, z_state, z_rows, e) for e in range(3)] + [item(e < x, x_state, x_rows, e) for e in range(3)]
    )
    peak_in = jnp.maximum(peak_all, total_all)
    rescale = jnp.exp(peak_all - peak_in)
    norm = norm * rescale
    state = state * jnp.where(row < 64, rescale[:, 0:1], rescale[:, 64:65])
    s_hi = state.astype(BF16)
    s_lo = (state - s_hi.astype(F32)).astype(BF16)
    for j in range(2):
        il = cum_col[:, j : j + 1] + peak_in[:, 64 * j : 64 * j + 1]
        m = row_s[j, :, 0:1]
        pr = jnp.maximum(il, m)
        e1, e2 = jnp.exp(m - pr), jnp.exp(il - pr)
        numer = e1 * num_s[j] + e2 * (mm(q_h[j], s_hi) + mm(q_h[j], s_lo))
        denom = e1 * row_s[j, :, 1:2] + e2 * jnp.sum(q_h[j].astype(F32) * norm, axis=1, keepdims=True)
        cell = numer / jnp.maximum(jnp.abs(denom), jnp.exp(-pr))
        mean = jnp.mean(cell * cell, axis=1, keepdims=True)
        cols = slice(j * 128, (j + 1) * 128)
        g = cell * lax.rsqrt(mean + 1e-06) * hg_ref[cols].astype(F32)[None, :] * jax.nn.sigmoid(og_ref[:, cols].astype(F32))
        gated[:, cols] = g.astype(BF16)

    local_wout.wait()
    local_res.wait()
    def cols_of(i):
        return slice(i * CH, (i + 1) * CH)

    for i in range(4):
        for n in range(2):
            r = mm(gated[...], wout[:, cols_of(2 * i + n)]).astype(BF16)
            part[i, :, n] = r.reshape(4, 2, ROWS, CH)
        send(("ad", i), part.at[i, :, :, oc], a_d2d.at[i], core)
    for i in range(4):
        arrived(("ad", i), a_d2d.at[i])
        f_sum[4 + i] = (part[i, :, :, c].astype(F32) + a_d2d[i].astype(F32)).astype(BF16)
        send(("a1l", i), f_sum.at[4 + i, yo, :, 0:32], a_r1.at[i, 0], y_right)
        send(("a1r", i), f_sum.at[4 + i, yo, :, 32:64], a_r1.at[i, 1], y_left)
    z_pass("gu", "p")
    for i in range(4):
        arrived(("a1l", i), a_r1.at[i, 0])
        f_sum[4 + i, yr, :, 0:32] = (f_sum[4 + i, yr, :, 0:32].astype(F32) + a_r1[i, 0].astype(F32)).astype(BF16)
        send(("a2l", i), f_sum.at[4 + i, yr], a_r2.at[i, 0], y_right, ("a2", i))
        arrived(("a1r", i), a_r1.at[i, 1])
        f_sum[4 + i, yl, :, 32:64] = (f_sum[4 + i, yl, :, 32:64].astype(F32) + a_r1[i, 1].astype(F32)).astype(BF16)
        send(("a2r", i), f_sum.at[4 + i, yl], a_r2.at[i, 1], y_left, ("a2", i))
    z_own_forward("gu")
    z_pass("gu", "q")
    square = jnp.zeros((ROWS, 1), F32)
    for i in range(4):
        arrived(("a2", i), a_r2.at[i])
        for n in range(2):
            cols = cols_of(2 * i + n)
            s = part[i, y, n, c].astype(F32) + a_d2d[i, y, n].astype(F32)
            s = s + a_r2[i, 0, n].astype(F32) + a_r2[i, 1, n].astype(F32) + res[:, cols].astype(F32)
            stream[:, cols] = s
            square = square + jnp.sum(s * s, axis=1, keepdims=True)
    scale = lax.rsqrt(square * (1.0 / D) + 1e-06)
    for i in range(8):
        cols = cols_of(i)
        nrm[y, h, c, :, cols] = (stream[:, cols] * scale * fgain_ref[cols].astype(F32)[None, :]).astype(BF16)

    def rows_of(yy, pp, cc, half=None):
        ref = nrm.at[yy, pp, cc]
        return ref if half is None else ref.at[half * 32 : (half + 1) * 32]

    def pass_on(key, yy, pp, dev, half=None):
        send(key, rows_of(yy, pp, c, half), rows_of(yy, pp, c, half), dev)

    pass_on(("ny", 0, "l"), y, h, y_right)
    pass_on(("ny", 0, "r"), y, h, y_left)
    pass_on(("nx",), y, h, x_pair)
    pass_on(("nc", 0, 0), y, h, core)
    z_other_forward("gu")
    for turn in ("l", "r"):
        x_pass("gu", turn, "p", "q", "o")
    x_own("d", "p", "q")
    z_pass("gu", "o")
    for s in range(1, 4):
        @pl.when(z + s < 4)
        def _():
            for d in z_state_copies(s):
                d.wait_send()
    drain(("xs",), ("xt",), ("ad",), ("a1l",), ("a1r",), ("a2l",), ("a2r",), ("zb", "gu"), ("z", "gu", "s"), ("x", "gu"))
    arrived(("nx",), rows_of(y, oh, c))
    pass_on(("ny", 1, "l"), y, oh, y_right)
    pass_on(("ny", 1, "r"), y, oh, y_left)
    pass_on(("nc", 0, 1), y, oh, core)

    def ring_forward(n, pp):
        arrived(("ny", n, "l"), rows_of(yl, pp, c))
        pass_on(("nf", n, "l"), yl, pp, y_right, 0)
        pass_on(("nc", 1, n), yl, pp, core)
        arrived(("ny", n, "r"), rows_of(yr, pp, c))
        pass_on(("nf", n, "r"), yr, pp, y_left, 1)
        pass_on(("nc", 2, n), yr, pp, core)

    def ring_last(n, pp):
        arrived(("nf", n, "l"), rows_of(yo, pp, c, 0))
        arrived(("nf", n, "r"), rows_of(yo, pp, c, 1))
        pass_on(("nc", 3, n), yo, pp, core)

    def from_core(place, yy):
        arrived(("nc", place, 0), rows_of(yy, h, oc))
        arrived(("nc", place, 1), rows_of(yy, oh, oc))

    def gu_tile(yy, kz, first):
        xs = nrm[yy, :, :, :, pl.ds(pl.multiple_of(kz * 1024, 1024), 1024)].reshape(256, 1024)
        for lo, hi in ((0, 512), (512, 1024), (1024, 1408)):
            r = mm(xs, gu_w[pl.ds(kz * 4, 4), :, lo:hi].reshape(1024, hi - lo))
            pre[yy, :, lo:hi] = r if first else pre[yy, :, lo:hi] + r

    def nth(base, i):
        return (base + i + i // 2 - 2 * (i // 3)) % 4

    ring_forward(0, h)
    z_pass_forward("gu", "p")
    from_core(0, y)
    gu_tile(y, z, True)
    drain(("zb",), ("nx",), ("ny", 0), ("nc", 0), ("z", "gu", "p"), ("f", "gu", "s"))
    z_pass_forward("gu", "q")
    z_far_own("gu")
    z_far_other("gu")
    x_pass("gu", "o", "p", "q", "o")
    x_own("d", "o")
    ring_forward(1, oh)
    from_core(1, yl)
    from_core(2, yr)

    @pl.loop(0, 2)
    def _(i):
        gu_tile((y + 1 + 2 * i) % 4, z, True)

    ring_last(0, h)
    z_pass_forward("gu", "o")
    z_other("d")
    z_own("d")
    z_pass("d", "p")
    z_pass("d", "q")
    x_done("gu", "l", "p", "q", "o")

    @pl.loop(0, 3)
    def _(i):
        gu_tile((y + i + i // 2) % 4, zl, False)

    ring_last(1, oh)
    x_done("gu", "r", "p", "q", "o")

    @pl.loop(0, 3)
    def _(i):
        gu_tile((y + i + i // 2) % 4, zr, False)

    from_core(3, yo)
    gu_tile(yo, z, True)

    @pl.loop(0, 2)
    def _(i):
        gu_tile(yo, (z + 1 + 2 * i) % 4, False)

    drain(("ny",), ("nf",), ("nc",), ("z", "gu"), ("fb",), ("x", "d", "p"), ("x", "d", "q"), ("xb", "gu"))
    drain(("f", "gu", "p"), ("f", "gu", "q"))
    z_done("gu", "p", "q")
    x_done("gu", "o", "p", "q", "o")

    def gu_slot(yy, zz, xx):
        k = zz * 4 + xx
        xs = nrm[yy, :, :, :, pl.ds(pl.multiple_of(k * 256, 256), 256)].reshape(256, 256)
        for lo, hi in ((0, 512), (512, 1024), (1024, 1408)):
            pre[yy, :, lo:hi] += mm(xs, gu_w[k, :, lo:hi])

    @pl.loop(0, 4)
    def _(yy):
        for xx in (x, xp, xq):
            gu_slot(yy, zo, xx)

    z_done("gu", "o")

    @pl.loop(0, 4)
    def _(yy):
        gu_slot(yy, zo, xo)
        rows = pl.ds(pl.multiple_of(yy * 256, 256), 256)
        hid[rows, 0:MAIN] = (jax.nn.silu(pre[yy, :, 0:MAIN]) * pre[yy, :, PADDED:WIDE]).astype(BF16)
        tail = pre[yy, :, MAIN:PADDED]
        both = jax.nn.silu(tail) * pltpu.roll(tail, 64, 1)
        hid[rows, MAIN:PADDED] = jnp.where(low == (h == 0), both, 0.0).astype(BF16)

    near, away = x // 2, 1 - x // 2
    order = [(z, near), (z, away), (zl, near), (zr, near), (zl, away), (zr, away), (zo, near), (zo, away)]

    def down(i):
        zz, j = order[i]
        if i >= 4:
            sent(("fd", i - 4))

        @pl.loop(0, 2)
        def _(s):
            r = nt(hid[...], d_w[zz * 4 + j * 2 + s]).astype(BF16)
            part[i % 4, :, :, :, :, pl.ds(pl.multiple_of(s * 256, 256), 256)] = r.reshape(4, 2, 2, ROWS, 256)

        send(("fd", i), part.at[i % 4, :, :, oc], f_d2d.at[i], core)

    def sum_cores(i):
        arrived(("fd", i), f_d2d.at[i])
        f_sum[i] = (part[i % 4, :, :, c].astype(F32) + f_d2d[i].astype(F32)).astype(BF16)
        send(("f1l", i), f_sum.at[i, yo, :, 0:32], f_r1.at[i, 0], y_right)
        send(("f1r", i), f_sum.at[i, yo, :, 32:64], f_r1.at[i, 1], y_left)

    def sum_far(i):
        arrived(("f1l", i), f_r1.at[i, 0])
        f_sum[i, yr, :, 0:32] = (f_sum[i, yr, :, 0:32].astype(F32) + f_r1[i, 0].astype(F32)).astype(BF16)
        send(("f2l", i), f_sum.at[i, yr], f_r2.at[i, 0], y_right, ("f2", i))
        arrived(("f1r", i), f_r1.at[i, 1])
        f_sum[i, yl, :, 32:64] = (f_sum[i, yl, :, 32:64].astype(F32) + f_r1[i, 1].astype(F32)).astype(BF16)
        send(("f2r", i), f_sum.at[i, yl], f_r2.at[i, 1], y_left, ("f2", i))

    def ring_sum(i, pp):
        return f_sum[i, y, pp].astype(F32) + f_r2[i, 0, pp].astype(F32) + f_r2[i, 1, pp].astype(F32)

    def sum_near(i):
        if i >= 2:
            drain(("f1l", i - 1), ("f1r", i - 1), ("f2l", i - 2), ("f2r", i - 2), ("fx", i - 2))
        arrived(("f2", i), f_r2.at[i])
        f_sum[i, y, oh] = ring_sum(i, oh).astype(BF16)
        send(("fx", i), f_sum.at[i, y, oh], f_xr.at[i], x_pair)

    def finish(i):
        zz, j = order[i]
        arrived(("fx", i), f_xr.at[i])
        cols = pl.ds(pl.multiple_of(zz * 1024 + j * CH, CH), CH)
        out_ref[:, cols] = (stream[:, cols] + 0.5 * (ring_sum(i, h) + f_xr[i].astype(F32))).astype(BF16)

    z_other_forward("d")
    for turn in ("l", "r"):
        x_pass("d", turn, "p", "q")
    down(0)
    z_pass("d", "o")
    down(1)
    sum_cores(0)
    z_own_forward("d")
    for turn in ("l", "r"):
        x_pass("d", turn, "o")
    sum_cores(1)
    sum_far(0)
    z_pass_forward("d", "p")
    sum_far(1)
    x_done("d", "l", "p")
    down(2)
    x_done("d", "r", "p")
    down(3)
    sum_near(0)
    sum_cores(2)
    z_pass_forward("d", "q")
    sum_cores(3)
    z_far_other("d")
    x_pass("d", "o", "p", "q")
    sum_far(2)
    z_pass_forward("d", "o")
    x_done("d", "l", "q", "o")
    down(4)
    sum_far(3)
    x_done("d", "r", "q", "o")
    down(5)
    sum_near(1)
    z_far_own("d")
    x_pass("d", "o", "o")
    sum_cores(4)
    sum_cores(5)
    drain(("x", "d"), ("z", "d"), ("f", "gu"), ("xb", "d", "l"), ("xb", "d", "r"), ("f", "d", "s"))
    z_done("d", "p")
    x_done("d", "o", "p")
    down(6)
    sum_far(4)
    sum_near(2)
    sum_cores(6)
    z_done("d", "q", "o")
    x_done("d", "o", "q", "o")
    down(7)
    sum_far(5)
    sum_near(3)
    sum_cores(7)
    sum_far(6)
    sum_near(4)
    sum_far(7)
    finish(0)
    finish(1)
    sum_near(5)
    for i in range(2, 6):
        finish(i)
    sum_near(6)
    sum_near(7)
    finish(6)
    drain(("f",), ("xb",), ("fd",))
    finish(7)

    for key in list(pending):
        sent(key)


def per_device(
    residual, queries, keys, values, output_gate, input_gate, forget_gate, extra_forget, head_gain, wout, ffn_gain,
    gate_w, up_w, down_w,
):
    vmem = pl.BlockSpec(memory_space=pltpu.VMEM)
    anywhere = pl.BlockSpec(memory_space=pl.ANY)
    scratch = [
        pltpu.VMEM((TOK, 128), BF16),
        pltpu.VMEM((TOK, 128), BF16),
        pltpu.VMEM((TOK, 256), BF16),
        pltpu.VMEM((TOK, 256), BF16),
        pltpu.VMEM((2, TOK), F32),
        pltpu.VMEM((2, TOK), F32),
        pltpu.VMEM((2, TOK), F32),
        pltpu.VMEM((256,), BF16),
        pltpu.VMEM((D,), BF16),
        pltpu.VMEM((16, 256, WIDE), BF16),
        pltpu.VMEM((16, 256, PADDED), BF16),
        pltpu.VMEM((256, WIDE), BF16),
        pltpu.VMEM((256, PADDED), BF16),
        pltpu.VMEM((3, 256 - SPLIT["gu"], WIDE), BF16),
        pltpu.VMEM((3, 256 - SPLIT["d"], PADDED), BF16),
        pltpu.VMEM((2, 256, 128), BF16),
        pltpu.VMEM((256, D), BF16),
        pltpu.VMEM((ROWS, D), BF16),
        pltpu.VMEM((4, 2, 2, ROWS, D), BF16),
        pltpu.VMEM((4, 256, WIDE), F32),
        pltpu.VMEM((1024, PADDED), BF16),
        pltpu.VMEM((4, 4, 2, 2, ROWS, CH), BF16),
        pltpu.VMEM((4, 4, 2, ROWS, CH), BF16),
        pltpu.VMEM((4, 2, 2, 32, CH), BF16),
        pltpu.VMEM((4, 2, 2, ROWS, CH), BF16),
        pltpu.VMEM((ROWS, D), F32),
        pltpu.VMEM((TOK, 256), BF16),
        pltpu.VMEM((8, 4, 2, ROWS, CH), BF16),
        pltpu.VMEM((8, 4, 2, ROWS, CH), BF16),
        pltpu.VMEM((8, 2, 2, 32, CH), BF16),
        pltpu.VMEM((8, 2, 2, ROWS, CH), BF16),
        pltpu.VMEM((8, ROWS, CH), BF16),
        pltpu.VMEM((4, 128, 128), F32),
        pltpu.VMEM((4, 8, 128), F32),
        pltpu.VMEM((4, 128, 128), F32),
        pltpu.VMEM((4, 8, 128), F32),
        pltpu.VMEM((2, TOK, 128), F32),
        pltpu.VMEM((2, TOK, 2), F32),
        pltpu.VMEM((8, TOK), F32),
        pltpu.SemaphoreType.DMA((NSEND,)),
        pltpu.SemaphoreType.DMA((NSEM,)),
        pltpu.SemaphoreType.DMA((2, 4)),
        pltpu.SemaphoreType.DMA((2, 4)),
        pltpu.SemaphoreType.DMA((21,)),
    ]
    return pl.pallas_call(
        kernel,
        out_shape=jax.ShapeDtypeStruct((ROWS, D), BF16),
        in_specs=[anywhere] * 14,
        out_specs=vmem,
        scratch_shapes=scratch,
        compiler_params=pltpu.CompilerParams(
            collective_id=0, has_side_effects=True, vmem_limit_bytes=67_043_328
        ),
        name="layer",
    )(
        queries, keys, values, output_gate, input_gate, forget_gate, extra_forget,
        head_gain, ffn_gain, wout, residual, gate_w, up_w, down_w,
    )


def solution(mesh):
    tp_sp = P("tp", "sp")
    rows = P("sp", "tp")
    in_specs = (
        P("sp", None), rows, rows, rows, rows, tp_sp, tp_sp, tp_sp, P("tp"), P("tp", None), P(), rows, rows, rows,
    )
    return jax.shard_map(
        per_device, mesh=mesh, in_specs=in_specs, out_specs=P(("sp", "tp"), None), check_vma=False
    )
```
